32 devices in a mesh: kv: 4 (over y, x), tp: 8 (over z, core).
Axes of the slice: x: 2, y: 2, z: 4, core: 2. Of those that a mesh axis runs over, the one named last changes fastest.
Arguments:
- residual: bfloat16 [128, 4096], P(None, ('kv', 'tp')), may hold values from -20 to 20
- mixer_gain: float32 [4096], P('kv'), may hold values from 0.1 to 1.9
- w_query: bfloat16 [4096, 4096], P('kv', 'tp'), may hold values from -0.09375 to 0.09375
- w_forget: bfloat16 [4096, 4096], P('kv', 'tp'), may hold values from -0.09375 to 0.09375
- w_input: bfloat16 [4096, 4096], P('kv', 'tp'), may hold values from -0.09375 to 0.09375
- w_outgate: bfloat16 [4096, 4096], P('kv', 'tp'), may hold values from -0.09375 to 0.09375
- lower_bound: float32 [4096], P('tp'), may hold values from 0.3 to 0.97
- state: float32 [128, 32, 128, 128], P('kv', 'tp'), may hold values from -6 to 6
- head_gain: float32 [128], replicated, may hold values from 0.1 to 1.9
- w_mix_out: bfloat16 [4096, 4096], P('tp', 'kv'), may hold values from -0.09375 to 0.09375
- ffn_gain: float32 [4096], P('kv'), may hold values from 0.1 to 1.9
- w_gate: bfloat16 [4096, 10752], P('kv', 'tp'), may hold values from -0.09375 to 0.09375
- w_up: bfloat16 [4096, 10752], P('kv', 'tp'), may hold values from -0.09375 to 0.09375
- w_down: bfloat16 [10752, 4096], P('tp', 'kv'), may hold values from -0.0625 to 0.0625
Outputs:
- layer_out: bfloat16 [128, 4096], P(None, ('kv', 'tp'))
- new_state: float32 [128, 32, 128, 128], P('kv', 'tp')
The draws below stay inside these ranges and needn't reach their ends.
All inputs are finite; a program needn't handle non-finite values.
Results may differ from the reference program's by a relative error of at most 0.015.
Values may be sent and summed in bfloat16 or wider, within the bound.
A program may use at most 64 MiB of HBM per device.

```python
import jax
import jax.numpy as jnp
from jax import lax

D = 4096
HEADS = 32
DK = 128
DV = 128
FF = 10752
SEQS = 128
HID = 4096
VID = 4096
N_KV = 4
N_TP = 8


def draw_residual(key, part):
    first = jax.random.fold_in(jax.random.fold_in(key, 11), 0)
    column = jnp.arange(D)
    kv_index = (column // (D // N_KV)).astype(jnp.float32)
    tp_index = (column // (D // (N_KV * N_TP)) % N_TP).astype(jnp.float32)
    col_scale = 0.4 * 3.0 ** (kv_index / max(N_KV - 1, 1)) * 3.0 ** (tp_index / max(N_TP - 1, 1))
    values = jnp.clip(jax.random.normal(first, (SEQS, D), jnp.float32), -4.0, 4.0)
    return jnp.clip(values * col_scale, -20.0, 20.0).astype(jnp.bfloat16)


def block_scale(stream_key, extent, pieces, smallest, high):
    gain = 1.0
    for position, shards_of in pieces:
        heights = jax.random.uniform(jax.random.fold_in(jax.random.fold_in(stream_key, 6), position), (shards_of,), jnp.float32, smallest / len(pieces), high / len(pieces))
        gain = gain * jnp.repeat(jnp.exp(heights), extent[position] // shards_of).reshape((-1,) + (1,) * (len(extent) - 1 - position))
    return gain


def scatter_about(stream_key, dims, scale, most, cuts=(), held_as=jnp.bfloat16):
    drawn = scale * jax.random.normal(stream_key, dims, jnp.float32)
    if cuts:
        drawn = drawn * block_scale(stream_key, dims, cuts, -0.22, 0.18)
    return jnp.clip(drawn, -most, most).astype(held_as)


def setup_inputs(seed: int = 0) -> dict:
    key_of = jax.random.split(jax.random.key(seed), 15)
    return {
        "residual": draw_residual(jax.random.fold_in(key_of[14], 71), 0),
        "mixer_gain": jnp.clip(1.0 + 0.18 * jax.random.normal(key_of[1], (D,), jnp.float32), 0.1, 1.9),
        "w_query": scatter_about(key_of[2], (D, HID), D ** -0.5, 0.09375, ((0, 4), (1, 8))),
        "w_forget": scatter_about(key_of[3], (D, HID), D ** -0.5, 0.09375, ((0, 4), (1, 8))),
        "w_input": scatter_about(key_of[4], (D, VID), D ** -0.5, 0.09375, ((0, 4), (1, 8))),
        "w_outgate": scatter_about(key_of[5], (D, VID), D ** -0.5, 0.09375, ((0, 4), (1, 8))),
        "lower_bound": jnp.clip(0.3 + 0.67 * jax.random.uniform(key_of[6], (HID,), jnp.float32) ** block_scale(key_of[6], (HID,), ((0, 8),), -0.2, 0.2), 0.3, 0.97),
        "state": scatter_about(key_of[7], (SEQS, HEADS, DK, DV), 1.0, 6.0, ((0, 4), (1, 8)), jnp.float32),
        "head_gain": jnp.clip(1.0 + 0.18 * jax.random.normal(key_of[8], (DV,), jnp.float32), 0.1, 1.9),
        "w_mix_out": scatter_about(key_of[9], (VID, D), VID ** -0.5, 0.09375, ((0, 8), (1, 4))),
        "ffn_gain": jnp.clip(1.0 + 0.18 * jax.random.normal(key_of[10], (D,), jnp.float32), 0.1, 1.9),
        "w_gate": scatter_about(key_of[11], (D, FF), D ** -0.5, 0.09375, ((0, 4), (1, 8))),
        "w_up": scatter_about(key_of[12], (D, FF), D ** -0.5, 0.09375, ((0, 4), (1, 8))),
        "w_down": scatter_about(key_of[13], (FF, D), FF ** -0.5, 0.0625, ((0, 8), (1, 4))),
    }


EPS = 1e-06

def reference(residual, mixer_gain, w_query, w_forget, w_input, w_outgate, lower_bound, state, head_gain, w_mix_out, ffn_gain, w_gate, w_up, w_down):
    seqs = residual.shape[0]
    xf = residual.astype(jnp.float32)
    inv_a = lax.rsqrt(lax.optimization_barrier(jnp.mean(xf * xf, axis=1, keepdims=True)) + EPS)
    scaled_a = (xf * mixer_gain).astype(jnp.bfloat16)
    query_raw = inv_a * jnp.dot(scaled_a, w_query, preferred_element_type=jnp.float32)
    forget_raw = inv_a * jnp.dot(scaled_a, w_forget, preferred_element_type=jnp.float32)
    value_raw = inv_a * jnp.dot(scaled_a, w_input, preferred_element_type=jnp.float32)
    outgate_raw = inv_a * jnp.dot(scaled_a, w_outgate, preferred_element_type=jnp.float32)
    bound = lower_bound.reshape(HEADS, DK)
    forget_raw = forget_raw.reshape(seqs, HEADS, DK)
    forget = bound + (1.0 - bound) * jax.nn.sigmoid(forget_raw)
    keyvec = (1.0 - bound) * jax.nn.sigmoid(-forget_raw)
    query = jax.nn.silu(query_raw.reshape(seqs, HEADS, DK))
    values = value_raw.reshape(seqs, HEADS, DV)
    new_state = forget[..., None] * state + keyvec[..., None] * values[:, :, None, :]
    head_out = jnp.einsum('shc,shce->she', query, new_state, precision=lax.Precision.HIGHEST)
    inv_h = lax.rsqrt(lax.optimization_barrier(jnp.mean(head_out * head_out, axis=2, keepdims=True)) + EPS)
    normed = head_out * inv_h * head_gain * jax.nn.silu(outgate_raw.reshape(seqs, HEADS, DV))
    normed = normed.reshape(seqs, HEADS * DV).astype(jnp.bfloat16)
    after_mix = (xf + jnp.dot(normed, w_mix_out, preferred_element_type=jnp.float32)).astype(jnp.bfloat16)
    af = after_mix.astype(jnp.float32)
    inv_b = lax.rsqrt(lax.optimization_barrier(jnp.mean(af * af, axis=1, keepdims=True)) + EPS)
    scaled_b = (af * ffn_gain).astype(jnp.bfloat16)
    gate = inv_b * jnp.dot(scaled_b, w_gate, preferred_element_type=jnp.float32)
    upper = inv_b * jnp.dot(scaled_b, w_up, preferred_element_type=jnp.float32)
    hidden = (jax.nn.silu(gate) * upper).astype(jnp.bfloat16)
    layer_out = (af + jnp.dot(hidden, w_down, preferred_element_type=jnp.float32)).astype(jnp.bfloat16)
    return (layer_out, new_state)
```

```python
import functools

import jax
import jax.numpy as jnp
from jax import lax
from jax.experimental import pallas as pl
from jax.experimental.pallas import tpu as pltpu
from jax.sharding import PartitionSpec as P

EPS = 1e-06
F32 = jnp.float32
BF16 = jnp.bfloat16
LANES = 128


def ring(axis, size):
    me = lax.axis_index(axis)
    return me, [lax.rem(me + step, size) for step in range(1, size)]


def greet(axes):
    barrier = pltpu.get_barrier_semaphore()
    count = 0
    for axis, peers in axes:
        for peer in peers:
            pl.semaphore_signal(
                barrier, inc=1, device_id={axis: peer}, device_id_type=pl.DeviceIdType.MESH
            )
            count += 1
    pl.semaphore_wait(barrier, count)


def remote(source, target, send_sem, recv_sem, axis, peer):
    return pltpu.make_async_remote_copy(
        src_ref=source,
        dst_ref=target,
        send_sem=send_sem,
        recv_sem=recv_sem,
        device_id={axis: peer},
        device_id_type=pl.DeviceIdType.MESH,
    )


def pairs(n_tp):
    me = lax.axis_index("tp")
    core = lax.rem(me, 2)
    return me, core, lax.div(me, 2), me + 1 - 2 * core, n_tp // 2


def start_gather(n_tp, source, blocks, send, recv):
    me, _, _, partner, half = pairs(n_tp)
    targets = [lax.rem(me + 2 * i, n_tp) for i in range(1, half)] + [partner]
    direct = [
        remote(source, blocks.at[me], send.at[i], recv.at[i], "tp", target)
        for i, target in enumerate(targets)
    ]
    for copy in direct:
        copy.start()
    blocks[pl.ds(me, 1)] = source[...][None]
    return direct


def relay_gather(n_tp, blocks, direct, send, recv):
    me, _, _, partner, half = pairs(n_tp)
    relays = []
    for i in range(1, half):
        origin = lax.rem(me - 2 * i + n_tp, n_tp)
        direct[i - 1].wait_recv()
        relay = remote(
            blocks.at[origin], blocks.at[origin],
            send.at[half + i - 1], recv.at[half + i - 1], "tp", partner,
        )
        relay.start()
        relays.append(relay)
    return relays


def end_gather(direct, relays):
    direct[-1].wait_recv()
    for relay in relays:
        relay.wait_recv()


def scale_block(blocks, gain_ref, scaled, count, width):
    squares = None
    for j in range(count):
        rows = blocks[j].astype(F32)
        cols = slice(j * width, (j + 1) * width)
        scaled[:, cols] = (rows * gain_ref[:, cols]).astype(BF16)
        term = rows * rows
        squares = term if squares is None else squares + term
    total = jnp.sum(squares, axis=1, keepdims=True)
    return jnp.broadcast_to(total, (total.shape[0], LANES))


def layer_kernel(
    n_kv, n_tp, features, parts_of,
    x_hbm, gain_a_hbm, gain_b_hbm, bound_hbm, head_gain_hbm,
    wq, wf, wi, wo, state_hbm, w_mix, w_gate, w_up, w_down,
    out_ref, fkv_ref,
    xs, gain_a, gain_b, bound, head_gain, proj_w, state, mix_w, gate_w, down_w,
    blocks, scaled, squares, squares_in, raws, raws_in, normed, heads_all,
    sums, pair_in, joined, sums_in, mixed,
    parts, parts_in, hidden, hiddens,
    x_sem, small_sem, proj_sem, state_sem, w_sem,
    g_send, g_recv, q_send, q_recv, r_send, r_recv, n_send, n_recv,
    t_send, t_recv, p_send, p_recv, h_send, h_recv,
):
    halves = range(parts_of)
    _, seqs, width = xs.shape
    rows = seqs // n_kv
    n_heads, depth, wide = proj_w.shape
    dk = wide // 4
    units = gate_w.shape[1]
    half = n_tp // 2

    x_loads = []
    for h in halves:
        for o in range(n_kv):
            x_loads.append(pltpu.make_async_copy(
                x_hbm.at[pl.ds((o * parts_of + h) * rows, rows), :],
                xs.at[h, pl.ds(o * rows, rows), :], x_sem.at[h, o],
            ))
    small_loads = [
        pltpu.make_async_copy(source, target, small_sem.at[i])
        for i, (source, target) in enumerate((
            (gain_a_hbm, gain_a), (gain_b_hbm, gain_b), (bound_hbm, bound), (head_gain_hbm, head_gain),
        ))
    ]
    proj_loads = [
        [
            pltpu.make_async_copy(
                source.at[:, pl.ds(j * dk, dk)], proj_w.at[j, :, pl.ds(p * dk, dk)], proj_sem.at[j, p]
            )
            for p, source in enumerate((wq, wf, wi, wo))
        ]
        for j in range(n_heads)
    ]
    state_loads = [
        pltpu.make_async_copy(
            state_hbm.at[pl.ds(h * rows, rows)], state.at[pl.ds(h * rows, rows)], state_sem.at[h]
        )
        for h in halves
    ]
    w_loads = [
        pltpu.make_async_copy(source, target, w_sem.at[i])
        for i, (source, target) in enumerate(
            ((w_mix, mix_w), (w_gate, gate_w.at[0]), (w_up, gate_w.at[1]), (w_down, down_w))
        )
    ]
    for load in x_loads + small_loads + sum(proj_loads, []) + state_loads + w_loads:
        load.start()

    kv, kv_peers = ring("kv", n_kv)
    me, core, chip, partner, _ = pairs(n_tp)
    own = pl.ds(pl.multiple_of(kv * rows, rows), rows)
    peer_rows = [pl.ds(pl.multiple_of(peer * rows, rows), rows) for peer in kv_peers]
    tp_peers = ring("tp", n_tp)[1]
    greet((("kv", kv_peers), ("tp", [partner] + tp_peers[1::2])))

    pending = []

    def send_squares(h, stage):
        copies = [
            remote(
                squares.at[stage, h, peer_rows[i], :], squares_in.at[stage, h, i],
                q_send.at[stage, h, i], q_recv.at[stage, h, i], "kv", peer,
            )
            for i, peer in enumerate(kv_peers)
        ]
        for copy in copies:
            copy.start()
        pending.extend(copies)
        return copies

    def inverse_of(h, stage, copies):
        total = squares[stage, h, own, :]
        for i, copy in enumerate(copies):
            copy.wait_recv()
            total = total + squares_in[stage, h, i]
        return lax.rsqrt(total[:, :1] / features + EPS)

    def spread(h, stage, source, target, send, recv):
        copies = [
            remote(source, target.at[h, own, :], send.at[h, i], recv.at[h, i], "kv", peer)
            for i, peer in enumerate(kv_peers)
        ]
        for copy in copies:
            copy.start()
        pending.extend(copies)
        target[h, own, :] = source[...]
        return copies

    group = max(1, 256 // width)
    while n_tp % group:
        group -= 1

    def start_reduce(h, stage, left, weight):
        for t in range(0, n_tp, group):
            part = jnp.dot(
                left[...], weight[:, t * width : (t + group) * width], preferred_element_type=F32
            ).astype(BF16)
            for j in range(group):
                sums[stage, h, (t + j) % 2, (t + j) // 2] = part[:, j * width : (j + 1) * width]
        first = remote(
            sums.at[stage, h, 1 - core], pair_in.at[stage, h],
            t_send.at[stage, h, 0], t_recv.at[stage, h, 0], "tp", partner,
        )
        first.start()
        pending.append(first)
        return first

    def pair_sum(h, stage, place):
        mine = sums[stage, h, pl.ds(core, 1), pl.ds(place, 1)][0, 0].astype(F32)
        return mine + pair_in[stage, h, pl.ds(place, 1)][0].astype(F32)

    def join_reduce(h, stage, first):
        first.wait_recv()
        out = []
        for i in range(1, half):
            joined[stage, h, i - 1] = pair_sum(h, stage, lax.rem(chip + i, half)).astype(BF16)
            copy = remote(
                joined.at[stage, h, i - 1], sums_in.at[stage, h, i - 1],
                t_send.at[stage, h, i], t_recv.at[stage, h, i], "tp", lax.rem(me + 2 * i, n_tp),
            )
            copy.start()
            out.append(copy)
        pending.extend(out)
        return out

    def end_reduce(h, stage, base, out):
        total = base + pair_sum(h, stage, chip)
        for i, copy in enumerate(out):
            copy.wait_recv()
            total = total + sums_in[stage, h, i].astype(F32)
        return total.astype(BF16)

    direct, relays, square_copies, copies = {}, {}, {}, {}

    for h in halves:
        for load in x_loads[h * n_kv : (h + 1) * n_kv]:
            load.wait()
        direct[h] = start_gather(n_tp, xs.at[h], blocks.at[0, h], g_send.at[0, h], g_recv.at[0, h])
        pending += direct[h]
    for load in small_loads:
        load.wait()
    for h in halves:
        relays[h] = relay_gather(n_tp, blocks.at[0, h], direct[h], g_send.at[0, h], g_recv.at[0, h])
        pending += relays[h]
    for h in halves:
        end_gather(direct[h], relays[h])
        squares[0, h] = scale_block(blocks.at[0, h], gain_a, scaled.at[0, h], n_tp, width)
        square_copies[h] = send_squares(h, 0)
        copies[h] = []
        for j in range(n_heads):
            if h == 0:
                for load in proj_loads[j]:
                    load.wait()
            raws[h, j] = jnp.dot(scaled[0, h], proj_w[j], preferred_element_type=F32).astype(BF16)
            sent = [
                remote(
                    raws.at[h, j, peer_rows[i], :], raws_in.at[h, i, j],
                    r_send.at[h, i, j], r_recv.at[h, i, j], "kv", peer,
                )
                for i, peer in enumerate(kv_peers)
            ]
            for copy in sent:
                copy.start()
            copies[h].append(sent)
            pending += sent

    spots = lax.broadcasted_iota(jnp.int32, (rows, dk), 0)
    for h in halves:
        inverse = inverse_of(h, 0, square_copies[h])
        state_loads[h].wait()
        for j in range(n_heads):
            cols = slice(j * dk, (j + 1) * dk)
            total = raws[h, j, own, :].astype(F32)
            for i, copy in enumerate(copies[h][j]):
                copy.wait_recv()
                total = total + raws_in[h, i, j].astype(F32)
            total = total * inverse
            query, raw, value, gate = (total[:, p * dk : (p + 1) * dk] for p in range(4))
            low = bound[:, cols]
            forget = low + (1.0 - low) * jax.nn.sigmoid(raw)
            keyvec = (1.0 - low) * jax.nn.sigmoid(-raw)
            query = query * jax.nn.sigmoid(query)
            fkv_ref[0, h, j] = forget
            fkv_ref[1, h, j] = keyvec
            fkv_ref[2, h, j] = value
            left = (query * forget).astype(BF16)
            head = jnp.sum(query * keyvec, axis=1, keepdims=True) * value
            for s in range(rows):
                seen = jnp.dot(left, state[h * rows + s, j].astype(BF16), preferred_element_type=F32)
                head = head + jnp.where(spots == s, seen, 0.0)
            scale = lax.rsqrt(jnp.mean(head * head, axis=1, keepdims=True) + EPS)
            normed[h, :, cols] = (
                head * scale * head_gain[...] * (gate * jax.nn.sigmoid(gate))
            ).astype(BF16)
        copies[h] = spread(h, 0, normed.at[h], heads_all, n_send, n_recv)

    firsts, outs = {}, {}
    w_loads[0].wait()
    for h in halves:
        for copy in copies[h]:
            copy.wait_recv()
        firsts[h] = start_reduce(h, 0, heads_all.at[h], mix_w)
    for h in halves:
        outs[h] = join_reduce(h, 0, firsts[h])
    for h in halves:
        mixed[h] = end_reduce(h, 0, xs[h].astype(F32), outs[h])
        direct[h] = start_gather(n_tp, mixed.at[h], blocks.at[1, h], g_send.at[1, h], g_recv.at[1, h])
        pending += direct[h]
    for h in halves:
        relays[h] = relay_gather(n_tp, blocks.at[1, h], direct[h], g_send.at[1, h], g_recv.at[1, h])
        pending += relays[h]
    step = min(512, units)
    for h in halves:
        end_gather(direct[h], relays[h])
        squares[1, h] = scale_block(blocks.at[1, h], gain_b, scaled.at[1, h], n_tp, width)
        square_copies[h] = send_squares(h, 1)
        copies[h] = []
        for g in range(2):
            if h == 0:
                w_loads[1 + g].wait()
            for c in range(0, units, step):
                end = min(c + step, units)
                parts[h, g, :, c:end] = lax.dot_general(
                    scaled[1, h], gate_w[g, c:end, :], (((1,), (1,)), ((), ())),
                    preferred_element_type=F32,
                ).astype(BF16)
            sent = [
                remote(
                    parts.at[h, g, peer_rows[i], :], parts_in.at[h, i, g],
                    p_send.at[h, i, g], p_recv.at[h, i, g], "kv", peer,
                )
                for i, peer in enumerate(kv_peers)
            ]
            for copy in sent:
                copy.start()
            copies[h].append(sent)
            pending += sent
    for h in halves:
        inverse = inverse_of(h, 1, square_copies[h])
        both = []
        for g in range(2):
            total = parts[h, g, own, :].astype(F32)
            for i, copy in enumerate(copies[h][g]):
                copy.wait_recv()
                total = total + parts_in[h, i, g].astype(F32)
            both.append(total * inverse)
        hidden[h] = (both[0] * jax.nn.sigmoid(both[0]) * both[1]).astype(BF16)
        copies[h] = spread(h, 1, hidden.at[h], hiddens, h_send, h_recv)
    w_loads[3].wait()
    for h in halves:
        for copy in copies[h]:
            copy.wait_recv()
        firsts[h] = start_reduce(h, 1, hiddens.at[h], down_w)
    for h in halves:
        outs[h] = join_reduce(h, 1, firsts[h])
    for h in halves:
        out_ref[h] = end_reduce(h, 1, mixed[h].astype(F32), outs[h])
    for copy in pending:
        copy.wait_send()


def split(value):
    high = value.astype(BF16).astype(F32)
    return high, value - high


def update_kernel(parts_of, n_kv, fkv_ref, state_ref, part_ref, new_ref, out_ref, news, picks, sems):
    _, _, n_heads, rows, dk = fkv_ref.shape
    for h in range(parts_of):
        for o in range(n_kv):
            out_ref[pl.ds((o * parts_of + h) * rows, rows), :] = part_ref[h, pl.ds(o * rows, rows), :]
    place = lax.broadcasted_iota(jnp.int32, (4 * rows, 2 * dk), 0)
    lane = lax.broadcasted_iota(jnp.int32, (4 * rows, 2 * dk), 1)
    side = jnp.where((place < 2 * rows) == (lane < dk), 1.0, 0.0)
    owner = lax.rem(place, rows)
    for s in range(rows):
        picks[s] = jnp.where(owner == s, side, 0.0).astype(BF16)

    def chunk(h, j):
        at = (pl.ds(h * rows, rows), pl.ds(j, 1))
        return pltpu.make_async_copy(news.at[at], new_ref.at[at], sems.at[h, j])

    for h in range(parts_of):
        def step(j, carry, h=h):
            left = jnp.concatenate(
                [*split(fkv_ref[0, h, j]), *split(fkv_ref[1, h, j])], axis=0
            ).T.astype(BF16)
            value = fkv_ref[2, h, j]
            for s in range(rows):
                wide = jnp.dot(left, picks[s], preferred_element_type=F32)
                news[h * rows + s, j] = (
                    wide[:, :dk] * state_ref[h * rows + s, j] + wide[:, dk:] * value[s : s + 1, :]
                )
            chunk(h, j).start()
            return carry
        lax.fori_loop(0, n_heads, step, 0)
    for h in range(parts_of):
        for j in range(n_heads):
            chunk(h, j).wait()


def in_vmem():
    return pl.BlockSpec(memory_space=pltpu.VMEM)


def in_hbm():
    return pl.BlockSpec(memory_space=pltpu.HBM)


def body(
    n_kv, n_tp,
    residual, mixer_gain, w_query, w_forget, w_input, w_outgate, lower_bound, state,
    head_gain, w_mix_out, ffn_gain, w_gate, w_up, w_down,
):
    seqs, width = residual.shape
    depth, hid = w_query.shape
    local, n_heads, dk, dv = state.shape
    units = w_gate.shape[1]
    features = depth * n_kv
    half = n_tp // 2
    parts_of = 2 if local % 32 == 0 else 1
    rows = local // parts_of
    some = seqs // parts_of
    dma = pltpu.SemaphoreType.DMA
    stay = lambda array: pltpu.with_memory_space_constraint(array, pltpu.HBM)
    held = pltpu.with_memory_space_constraint(state, pltpu.VMEM)

    part, fkv = pl.pallas_call(
        functools.partial(layer_kernel, n_kv, n_tp, features, parts_of),
        out_shape=(
            jax.ShapeDtypeStruct((parts_of, some, width), BF16),
            jax.ShapeDtypeStruct((3, parts_of, n_heads, rows, dk), F32),
        ),
        in_specs=[in_hbm()] * 14,
        out_specs=(in_vmem(), in_vmem()),
        scratch_shapes=[
            pltpu.VMEM((parts_of, some, width), BF16),
            pltpu.VMEM((1, depth), F32),
            pltpu.VMEM((1, depth), F32),
            pltpu.VMEM((1, hid), F32),
            pltpu.VMEM((1, dv), F32),
            pltpu.VMEM((n_heads, depth, 4 * dk), BF16),
            pltpu.VMEM(state.shape, F32),
            pltpu.VMEM(w_mix_out.shape, BF16),
            pltpu.VMEM((2, units, depth), BF16),
            pltpu.VMEM(w_down.shape, BF16),
            pltpu.VMEM((2, parts_of, n_tp, some, width), BF16),
            pltpu.VMEM((2, parts_of, some, depth), BF16),
            pltpu.VMEM((2, parts_of, some, LANES), F32),
            pltpu.VMEM((2, parts_of, n_kv - 1, rows, LANES), F32),
            pltpu.VMEM((parts_of, n_heads, some, 4 * dk), BF16),
            pltpu.VMEM((parts_of, n_kv - 1, n_heads, rows, 4 * dk), BF16),
            pltpu.VMEM((parts_of, rows, hid), BF16),
            pltpu.VMEM((parts_of, some, hid), BF16),
            pltpu.VMEM((2, parts_of, 2, half, some, width), BF16),
            pltpu.VMEM((2, parts_of, half, some, width), BF16),
            pltpu.VMEM((2, parts_of, half - 1, some, width), BF16),
            pltpu.VMEM((2, parts_of, half - 1, some, width), BF16),
            pltpu.VMEM((parts_of, some, width), BF16),
            pltpu.VMEM((parts_of, 2, some, units), BF16),
            pltpu.VMEM((parts_of, n_kv - 1, 2, rows, units), BF16),
            pltpu.VMEM((parts_of, rows, units), BF16),
            pltpu.VMEM((parts_of, some, units), BF16),
            dma((parts_of, n_kv)), dma((4,)), dma((n_heads, 4)), dma((parts_of,)), dma((4,)),
            dma((2, parts_of, n_tp - 1)), dma((2, parts_of, n_tp - 1)),
            dma((2, parts_of, n_kv - 1)), dma((2, parts_of, n_kv - 1)),
            dma((parts_of, n_kv - 1, n_heads)), dma((parts_of, n_kv - 1, n_heads)),
            dma((parts_of, n_kv - 1)), dma((parts_of, n_kv - 1)),
            dma((2, parts_of, half)), dma((2, parts_of, half)),
            dma((parts_of, n_kv - 1, 2)), dma((parts_of, n_kv - 1, 2)),
            dma((parts_of, n_kv - 1)), dma((parts_of, n_kv - 1)),
        ],
        compiler_params=pltpu.CompilerParams(
            collective_id=0, has_side_effects=True, vmem_limit_bytes=44 * 2**20
        ),
        name="layer",
    )(*map(stay, (
        residual, mixer_gain.reshape(1, depth), ffn_gain.reshape(1, depth),
        lower_bound.reshape(1, hid), head_gain.reshape(1, dv),
        w_query, w_forget, w_input, w_outgate, state, w_mix_out, w_gate.T, w_up.T, w_down,
    )))

    updated, layer_out = pl.pallas_call(
        functools.partial(update_kernel, parts_of, n_kv),
        out_shape=(
            jax.ShapeDtypeStruct(state.shape, F32),
            jax.ShapeDtypeStruct((seqs, width), BF16),
        ),
        in_specs=[in_vmem()] * 3,
        out_specs=(in_hbm(), in_vmem()),
        scratch_shapes=[
            pltpu.VMEM(state.shape, F32),
            pltpu.VMEM((rows, 4 * rows, 2 * dk), BF16),
            dma((parts_of, n_heads)),
        ],
        compiler_params=pltpu.CompilerParams(vmem_limit_bytes=44 * 2**20),
        name="update",
    )(fkv, held, part)
    return layer_out, updated


def solution(mesh):
    in_specs = (
        P(None, ("kv", "tp")),
        P("kv"),
        P("kv", "tp"),
        P("kv", "tp"),
        P("kv", "tp"),
        P("kv", "tp"),
        P("tp"),
        P("kv", "tp", None, None),
        P(),
        P("tp", "kv"),
        P("kv"),
        P("kv", "tp"),
        P("kv", "tp"),
        P("tp", "kv"),
    )
    out_specs = (P(None, ("kv", "tp")), P("kv", "tp", None, None))
    return jax.shard_map(
        functools.partial(body, mesh.shape["kv"], mesh.shape["tp"]),
        mesh=mesh, in_specs=in_specs, out_specs=out_specs, check_vma=False,
    )
```

```python
import functools

import jax
import jax.numpy as jnp
from jax import lax
from jax.experimental import pallas as pl
from jax.experimental.pallas import tpu as pltpu
from jax.sharding import PartitionSpec as P

EPS = 1e-06
F32 = jnp.float32
BF16 = jnp.bfloat16
LANES = 128


def ring(axis, size):
    me = lax.axis_index(axis)
    return me, [lax.rem(me + step, size) for step in range(1, size)]


def greet(axes):
    barrier = pltpu.get_barrier_semaphore()
    count = 0
    for axis, peers in axes:
        for peer in peers:
            pl.semaphore_signal(
                barrier, inc=1, device_id={axis: peer}, device_id_type=pl.DeviceIdType.MESH
            )
            count += 1
    pl.semaphore_wait(barrier, count)


def remote(source, target, send_sem, recv_sem, axis, peer):
    return pltpu.make_async_remote_copy(
        src_ref=source,
        dst_ref=target,
        send_sem=send_sem,
        recv_sem=recv_sem,
        device_id={axis: peer},
        device_id_type=pl.DeviceIdType.MESH,
    )


def pairs(n_tp):
    me = lax.axis_index("tp")
    core = lax.rem(me, 2)
    return me, core, lax.div(me, 2), me + 1 - 2 * core, n_tp // 2


def landed(ref, sem):
    pltpu.make_async_copy(ref, ref, sem).wait()


def start_gather(n_tp, source, blocks, send, recv):
    me, _, _, partner, half = pairs(n_tp)
    targets = [lax.rem(me + 2 * i, n_tp) for i in range(1, half)] + [partner]
    direct = [
        remote(source, blocks.at[me], send, recv.at[i], "tp", target)
        for i, target in enumerate(targets)
    ]
    for copy in direct:
        copy.start()
    blocks[pl.ds(me, 1)] = source[...][None]
    return direct


def relay_gather(n_tp, blocks, direct, send, recv):
    me, _, _, partner, half = pairs(n_tp)
    for i in range(1, half):
        origin = lax.rem(me - 2 * i + n_tp, n_tp)
        direct[i - 1].wait_recv()
        remote(
            blocks.at[origin], blocks.at[origin], send, recv.at[half - 1], "tp", partner
        ).start()


def end_gather(n_tp, blocks, recv):
    half = n_tp // 2
    landed(blocks.at[pl.ds(0, half)], recv.at[half - 1])


def scale_block(blocks, gain_ref, scaled, count, width):
    squares = None
    for j in range(count):
        rows = blocks[j].astype(F32)
        cols = slice(j * width, (j + 1) * width)
        scaled[:, cols] = (rows * gain_ref[:, cols]).astype(BF16)
        term = rows * rows
        squares = term if squares is None else squares + term
    total = jnp.sum(squares, axis=1, keepdims=True)
    return jnp.broadcast_to(total, (total.shape[0], LANES))


def split(value):
    high = value.astype(BF16).astype(F32)
    return high, value - high


def layer_kernel(
    n_kv, n_tp, features, parts_of,
    x_hbm, gain_a_hbm, gain_b_hbm, bound_hbm, head_gain_hbm,
    wq, wf, wi, wo, state_hbm, w_mix, w_gate, w_up, w_down,
    out_ref, state,
    xs, gain_a, gain_b, bound, head_gain, proj_w, state16, picks, fkv, mix_w, gate_w, down_w,
    blocks, scaled, squares, squares_in, raws, raws_in, normed, heads_all,
    sums, pair_in, joined, sums_in, mixed,
    parts, parts_in, hidden, hiddens,
    x_sem, small_sem, proj_sem, state_sem, w_sem,
    g_send, g_recv, q_send, q_recv, r_send, r_recv, n_send, n_recv,
    t_send, t_recv, p_send, p_recv, h_send, h_recv,
):
    halves = range(parts_of)
    _, seqs, width = xs.shape
    rows = seqs // n_kv
    n_heads, depth, wide = proj_w.shape
    dk = wide // 4
    units = gate_w.shape[1]
    half = n_tp // 2

    x_loads = []
    for h in halves:
        for o in range(n_kv):
            x_loads.append(pltpu.make_async_copy(
                x_hbm.at[pl.ds((o * parts_of + h) * rows, rows), :],
                xs.at[h, pl.ds(o * rows, rows), :], x_sem.at[h],
            ))
    small_loads = [
        pltpu.make_async_copy(source, target, small_sem.at[i])
        for i, (source, target) in enumerate((
            (gain_a_hbm, gain_a), (gain_b_hbm, gain_b), (bound_hbm, bound), (head_gain_hbm, head_gain),
        ))
    ]
    proj_loads = [
        [
            pltpu.make_async_copy(
                source.at[:, pl.ds(j * dk, dk)], proj_w.at[j, :, pl.ds(p * dk, dk)], proj_sem.at[j]
            )
            for p, source in enumerate((wq, wf, wi, wo))
        ]
        for j in range(n_heads)
    ]
    state_loads = [
        pltpu.make_async_copy(
            state_hbm.at[pl.ds(h * rows, rows)], state.at[pl.ds(h * rows, rows)], state_sem.at[h]
        )
        for h in halves
    ]
    w_loads = [
        pltpu.make_async_copy(source, target, w_sem.at[i])
        for i, (source, target) in enumerate(
            ((w_mix, mix_w), (w_gate, gate_w.at[0]), (w_up, gate_w.at[1]), (w_down, down_w))
        )
    ]
    for load in x_loads + small_loads + sum(proj_loads, []):
        load.start()

    kv, kv_peers = ring("kv", n_kv)
    me, core, chip, partner, _ = pairs(n_tp)
    own = pl.ds(pl.multiple_of(kv * rows, rows), rows)
    peer_rows = [pl.ds(pl.multiple_of(peer * rows, rows), rows) for peer in kv_peers]
    tp_peers = ring("tp", n_tp)[1]
    greet((("kv", kv_peers), ("tp", [partner] + tp_peers[1::2])))

    def send_squares(h, stage):
        for i, peer in enumerate(kv_peers):
            remote(
                squares.at[stage, h, peer_rows[i], :], squares_in.at[stage, h, i],
                q_send, q_recv.at[stage, h], "kv", peer,
            ).start()

    def inverse_of(h, stage):
        landed(squares_in.at[stage, h], q_recv.at[stage, h])
        total = squares[stage, h, own, :]
        for i in range(n_kv - 1):
            total = total + squares_in[stage, h, i]
        return lax.rsqrt(total[:, :1] / features + EPS)

    def spread(h, source, target, send, recv):
        for peer in kv_peers:
            remote(source, target.at[h, own, :], send, recv.at[h], "kv", peer).start()
        target[h, own, :] = source[...]

    def others(target):
        return target.at[pl.ds(0, (n_kv - 1) * rows), :]

    group = max(1, 256 // width)
    while n_tp % group:
        group -= 1

    def start_reduce(h, stage, left, weight):
        for t in range(0, n_tp, group):
            part = jnp.dot(
                left[...], weight[:, t * width : (t + group) * width], preferred_element_type=F32
            ).astype(BF16)
            for j in range(group):
                sums[stage, h, (t + j) % 2, (t + j) // 2] = part[:, j * width : (j + 1) * width]
        first = remote(
            sums.at[stage, h, 1 - core], pair_in.at[stage, h],
            t_send.at[0], t_recv.at[stage, h, 0], "tp", partner,
        )
        first.start()
        return first

    def pair_sum(h, stage, place):
        mine = sums[stage, h, pl.ds(core, 1), pl.ds(place, 1)][0, 0].astype(F32)
        return mine + pair_in[stage, h, pl.ds(place, 1)][0].astype(F32)

    def join_reduce(h, stage, first):
        first.wait_recv()
        for i in range(1, half):
            joined[stage, h, i - 1] = pair_sum(h, stage, lax.rem(chip + i, half)).astype(BF16)
            remote(
                joined.at[stage, h, i - 1], sums_in.at[stage, h, i - 1],
                t_send.at[1], t_recv.at[stage, h, 1], "tp", lax.rem(me + 2 * i, n_tp),
            ).start()

    def end_reduce(h, stage, base):
        total = base + pair_sum(h, stage, chip)
        landed(sums_in.at[stage, h], t_recv.at[stage, h, 1])
        for i in range(half - 1):
            total = total + sums_in[stage, h, i].astype(F32)
        return total.astype(BF16)

    direct = {}

    for h in halves:
        landed(xs.at[h], x_sem.at[h])
        direct[h] = start_gather(n_tp, xs.at[h], blocks.at[0, h], g_send.at[0], g_recv.at[0, h])
    place = lax.broadcasted_iota(jnp.int32, (4 * rows, 2 * dk), 0)
    lane = lax.broadcasted_iota(jnp.int32, (4 * rows, 2 * dk), 1)
    side = jnp.where((place < 2 * rows) == (lane < dk), 1.0, 0.0)
    owner = lax.rem(place, rows)
    for s in range(rows):
        picks[s] = jnp.where(owner == s, side, 0.0).astype(BF16)

    def update(h):
        def step(j, carry):
            left = jnp.concatenate(
                [*split(fkv[0, h, j]), *split(fkv[1, h, j])], axis=0
            ).T.astype(BF16)
            value = fkv[2, h, j]
            for s in range(rows):
                wide = jnp.dot(left, picks[s], preferred_element_type=F32)
                state[h * rows + s, j] = (
                    wide[:, :dk] * state[h * rows + s, j] + wide[:, dk:] * value[s : s + 1, :]
                )
            return carry
        lax.fori_loop(0, n_heads, step, 0)

    for load in small_loads:
        load.wait()
    for h in halves:
        relay_gather(n_tp, blocks.at[0, h], direct[h], g_send.at[0], g_recv.at[0, h])
    for load in state_loads:
        load.start()
    for h in halves:
        end_gather(n_tp, blocks.at[0, h], g_recv.at[0, h])
        squares[0, h] = scale_block(blocks.at[0, h], gain_a, scaled.at[0, h], n_tp, width)
        send_squares(h, 0)
        for j in range(n_heads):
            if h == 0:
                landed(proj_w.at[j], proj_sem.at[j])
            raws[h, j] = jnp.dot(scaled[0, h], proj_w[j], preferred_element_type=F32).astype(BF16)
            for i, peer in enumerate(kv_peers):
                remote(
                    raws.at[h, j, peer_rows[i], :], raws_in.at[h, j, i],
                    r_send, r_recv.at[h, j], "kv", peer,
                ).start()

    for load in w_loads:
        load.start()

    def narrow(h):
        def step(j, carry):
            for s in range(rows):
                state16[h, j, :, s * dk : (s + 1) * dk] = state[h * rows + s, j].astype(BF16)
            return carry
        lax.fori_loop(0, n_heads, step, 0)

    for h in halves:
        state_loads[h].wait()
        narrow(h)
    spots = lax.broadcasted_iota(jnp.int32, (rows, dk), 0)
    for h in halves:
        inverse = inverse_of(h, 0)
        for j in range(n_heads):
            cols = slice(j * dk, (j + 1) * dk)
            total = raws[h, j, own, :].astype(F32)
            landed(raws_in.at[h, j], r_recv.at[h, j])
            for i in range(n_kv - 1):
                total = total + raws_in[h, j, i].astype(F32)
            total = total * inverse
            query, raw, value, gate = (total[:, p * dk : (p + 1) * dk] for p in range(4))
            low = bound[:, cols]
            forget = low + (1.0 - low) * jax.nn.sigmoid(raw)
            keyvec = (1.0 - low) * jax.nn.sigmoid(-raw)
            query = query * jax.nn.sigmoid(query)
            fkv[0, h, j] = forget
            fkv[1, h, j] = keyvec
            fkv[2, h, j] = value
            left = (query * forget).astype(BF16)
            head = jnp.sum(query * keyvec, axis=1, keepdims=True) * value
            seen = jnp.dot(left, state16[h, j], preferred_element_type=F32)
            for s in range(rows):
                head = head + jnp.where(spots == s, seen[:, s * dk : (s + 1) * dk], 0.0)
            scale = lax.rsqrt(jnp.mean(head * head, axis=1, keepdims=True) + EPS)
            normed[h, :, cols] = (
                head * scale * head_gain[...] * (gate * jax.nn.sigmoid(gate))
            ).astype(BF16)
        spread(h, normed.at[h], heads_all, n_send, n_recv)

    w_loads[0].wait()
    for h in halves:
        landed(others(heads_all.at[h]), n_recv.at[h])
        join_reduce(h, 0, start_reduce(h, 0, heads_all.at[h], mix_w))
    for h in halves:
        mixed[h] = end_reduce(h, 0, xs[h].astype(F32))
        direct[h] = start_gather(n_tp, mixed.at[h], blocks.at[1, h], g_send.at[1], g_recv.at[1, h])
        if h == 0:
            update(0)

    def relay(h):
        relay_gather(n_tp, blocks.at[1, h], direct[h], g_send.at[1], g_recv.at[1, h])

    relay(0)
    step = min(512, units)
    chunks = [(c, min(c + step, units)) for c in range(0, units, step)]
    for h in halves:
        end_gather(n_tp, blocks.at[1, h], g_recv.at[1, h])
        squares[1, h] = scale_block(blocks.at[1, h], gain_b, scaled.at[1, h], n_tp, width)
        send_squares(h, 1)
        for k, (c, end) in enumerate(chunks):
            for g in range(2):
                if h == 0 and k == 0:
                    w_loads[1 + g].wait()
                parts[h, g, :, c:end] = lax.dot_general(
                    scaled[1, h], gate_w[g, c:end, :], (((1,), (1,)), ((), ())),
                    preferred_element_type=F32,
                ).astype(BF16)
                for i, peer in enumerate(kv_peers):
                    remote(
                        parts.at[h, g, peer_rows[i], c:end], parts_in.at[h, i, g, :, c:end],
                        p_send, p_recv.at[h], "kv", peer,
                    ).start()
            if k == len(chunks) // 2 and h + 1 < parts_of:
                relay(h + 1)
    for h in range(1, parts_of):
        update(h)
    for h in halves:
        inverse = inverse_of(h, 1)
        landed(parts_in.at[h], p_recv.at[h])
        both = []
        for g in range(2):
            total = parts[h, g, own, :].astype(F32)
            for i in range(n_kv - 1):
                total = total + parts_in[h, i, g].astype(F32)
            both.append(total * inverse)
        hidden[h] = (both[0] * jax.nn.sigmoid(both[0]) * both[1]).astype(BF16)
        if h == 0:
            landed(parts_in, p_send)
        spread(h, hidden.at[h], hiddens, h_send, h_recv)
    w_loads[3].wait()
    for h in halves:
        landed(others(hiddens.at[h]), h_recv.at[h])
        join_reduce(h, 1, start_reduce(h, 1, hiddens.at[h], down_w))
    for h in halves:
        out_ref[h] = end_reduce(h, 1, mixed[h].astype(F32))
    for stage in range(2):
        landed(blocks.at[stage, :, pl.ds(0, n_tp - 1)], g_send.at[stage])
    for ref, sem in (
        (squares_in, q_send), (raws_in, r_send), (pair_in, t_send.at[0]), (sums_in, t_send.at[1]),
        (heads_all.at[:, pl.ds(0, (n_kv - 1) * rows)], n_send),
        (hiddens.at[:, pl.ds(0, (n_kv - 1) * rows)], h_send),
    ):
        landed(ref, sem)


def deliver_kernel(parts_of, n_kv, state_ref, part_ref, new_ref, out_ref, sems):
    local = state_ref.shape[0]
    rows = local // parts_of
    count = sems.shape[0]
    some = local // count
    copies = [
        pltpu.make_async_copy(
            state_ref.at[pl.ds(i * some, some)], new_ref.at[pl.ds(i * some, some)], sems.at[i]
        )
        for i in range(count)
    ]
    for copy in copies:
        copy.start()
    for h in range(parts_of):
        for o in range(n_kv):
            out_ref[pl.ds((o * parts_of + h) * rows, rows), :] = part_ref[h, pl.ds(o * rows, rows), :]
    for copy in copies:
        copy.wait()


def in_vmem():
    return pl.BlockSpec(memory_space=pltpu.VMEM)


def in_hbm():
    return pl.BlockSpec(memory_space=pltpu.HBM)


def body(
    n_kv, n_tp,
    residual, mixer_gain, w_query, w_forget, w_input, w_outgate, lower_bound, state,
    head_gain, w_mix_out, ffn_gain, w_gate, w_up, w_down,
):
    seqs, width = residual.shape
    depth, hid = w_query.shape
    local, n_heads, dk, dv = state.shape
    units = w_gate.shape[1]
    features = depth * n_kv
    half = n_tp // 2
    parts_of = 2 if local % 32 == 0 else 1
    rows = local // parts_of
    some = seqs // parts_of
    dma = pltpu.SemaphoreType.DMA
    stay = lambda array: pltpu.with_memory_space_constraint(array, pltpu.HBM)

    part, held = pl.pallas_call(
        functools.partial(layer_kernel, n_kv, n_tp, features, parts_of),
        out_shape=(
            jax.ShapeDtypeStruct((parts_of, some, width), BF16),
            jax.ShapeDtypeStruct(state.shape, F32),
        ),
        in_specs=[in_hbm()] * 14,
        out_specs=(in_vmem(), in_vmem()),
        scratch_shapes=[
            pltpu.VMEM((parts_of, some, width), BF16),
            pltpu.VMEM((1, depth), F32),
            pltpu.VMEM((1, depth), F32),
            pltpu.VMEM((1, hid), F32),
            pltpu.VMEM((1, dv), F32),
            pltpu.VMEM((n_heads, depth, 4 * dk), BF16),
            pltpu.VMEM((parts_of, n_heads, dk, rows * dv), BF16),
            pltpu.VMEM((rows, 4 * rows, 2 * dk), BF16),
            pltpu.VMEM((3, parts_of, n_heads, rows, dk), F32),
            pltpu.VMEM(w_mix_out.shape, BF16),
            pltpu.VMEM((2, units, depth), BF16),
            pltpu.VMEM(w_down.shape, BF16),
            pltpu.VMEM((2, parts_of, n_tp, some, width), BF16),
            pltpu.VMEM((2, parts_of, some, depth), BF16),
            pltpu.VMEM((2, parts_of, some, LANES), F32),
            pltpu.VMEM((2, parts_of, n_kv - 1, rows, LANES), F32),
            pltpu.VMEM((parts_of, n_heads, some, 4 * dk), BF16),
            pltpu.VMEM((parts_of, n_heads, n_kv - 1, rows, 4 * dk), BF16),
            pltpu.VMEM((parts_of, rows, hid), BF16),
            pltpu.VMEM((parts_of, some, hid), BF16),
            pltpu.VMEM((2, parts_of, 2, half, some, width), BF16),
            pltpu.VMEM((2, parts_of, half, some, width), BF16),
            pltpu.VMEM((2, parts_of, half - 1, some, width), BF16),
            pltpu.VMEM((2, parts_of, half - 1, some, width), BF16),
            pltpu.VMEM((parts_of, some, width), BF16),
            pltpu.VMEM((parts_of, 2, some, units), BF16),
            pltpu.VMEM((parts_of, n_kv - 1, 2, rows, units), BF16),
            pltpu.VMEM((parts_of, rows, units), BF16),
            pltpu.VMEM((parts_of, some, units), BF16),
            dma((parts_of,)), dma((4,)), dma((n_heads,)), dma((parts_of,)), dma((4,)),
            dma((2,)), dma((2, parts_of, half)),
            dma, dma((2, parts_of)),
            dma, dma((parts_of, n_heads)),
            dma, dma((parts_of,)),
            dma((2,)), dma((2, parts_of, 2)),
            dma, dma((parts_of,)),
            dma, dma((parts_of,)),
        ],
        compiler_params=pltpu.CompilerParams(
            collective_id=0, has_side_effects=True, vmem_limit_bytes=44 * 2**20
        ),
        name="layer",
    )(*map(stay, (
        residual, mixer_gain.reshape(1, depth), ffn_gain.reshape(1, depth),
        lower_bound.reshape(1, hid), head_gain.reshape(1, dv),
        w_query, w_forget, w_input, w_outgate, state, w_mix_out, w_gate.T, w_up.T, w_down,
    )))

    held = pltpu.with_memory_space_constraint(held, pltpu.VMEM)
    updated, layer_out = pl.pallas_call(
        functools.partial(deliver_kernel, parts_of, n_kv),
        out_shape=(
            jax.ShapeDtypeStruct(state.shape, F32),
            jax.ShapeDtypeStruct((seqs, width), BF16),
        ),
        in_specs=[in_vmem()] * 2,
        out_specs=(in_hbm(), in_vmem()),
        scratch_shapes=[dma((8 if local % 8 == 0 else 1,))],
        compiler_params=pltpu.CompilerParams(vmem_limit_bytes=16 * 2**20),
        name="deliver",
    )(held, part)
    return layer_out, updated


def solution(mesh):
    in_specs = (
        P(None, ("kv", "tp")),
        P("kv"),
        P("kv", "tp"),
        P("kv", "tp"),
        P("kv", "tp"),
        P("kv", "tp"),
        P("tp"),
        P("kv", "tp", None, None),
        P(),
        P("tp", "kv"),
        P("kv"),
        P("kv", "tp"),
        P("kv", "tp"),
        P("tp", "kv"),
    )
    out_specs = (P(None, ("kv", "tp")), P("kv", "tp", None, None))
    return jax.shard_map(
        functools.partial(body, mesh.shape["kv"], mesh.shape["tp"]),
        mesh=mesh, in_specs=in_specs, out_specs=out_specs, check_vma=False,
    )
```

```python
import functools

import jax
import jax.numpy as jnp
from jax import lax
from jax.experimental import pallas as pl
from jax.experimental.pallas import tpu as pltpu
from jax.sharding import PartitionSpec as P

EPS = 1e-06
F32 = jnp.float32
BF16 = jnp.bfloat16
LANES = 128


def ring(axis, size):
    me = lax.axis_index(axis)
    return me, [lax.rem(me + step, size) for step in range(1, size)]


def greet(axes):
    barrier = pltpu.get_barrier_semaphore()
    count = 0
    for axis, peers in axes:
        for peer in peers:
            pl.semaphore_signal(
                barrier, inc=1, device_id={axis: peer}, device_id_type=pl.DeviceIdType.MESH
            )
            count += 1
    pl.semaphore_wait(barrier, count)


def remote(source, target, send_sem, recv_sem, axis, peer):
    return pltpu.make_async_remote_copy(
        src_ref=source,
        dst_ref=target,
        send_sem=send_sem,
        recv_sem=recv_sem,
        device_id={axis: peer},
        device_id_type=pl.DeviceIdType.MESH,
    )


def pairs(n_tp):
    me = lax.axis_index("tp")
    core = lax.rem(me, 2)
    return me, core, lax.div(me, 2), me + 1 - 2 * core, n_tp // 2


def landed(ref, sem):
    pltpu.make_async_copy(ref, ref, sem).wait()


def start_gather(n_tp, source, blocks, send, recv):
    me, _, _, partner, half = pairs(n_tp)
    targets = [lax.rem(me + 2 * i, n_tp) for i in range(1, half)] + [partner]
    direct = [
        remote(source, blocks.at[me], send, recv.at[i], "tp", target)
        for i, target in enumerate(targets)
    ]
    for copy in direct:
        copy.start()
    blocks[pl.ds(me, 1)] = source[...][None]
    return direct


def relay_gather(n_tp, blocks, direct, send, recv):
    me, _, _, partner, half = pairs(n_tp)
    for i in range(1, half):
        origin = lax.rem(me - 2 * i + n_tp, n_tp)
        direct[i - 1].wait_recv()
        remote(
            blocks.at[origin], blocks.at[origin], send, recv.at[half - 1], "tp", partner
        ).start()


def end_gather(n_tp, blocks, recv):
    half = n_tp // 2
    landed(blocks.at[pl.ds(0, half)], recv.at[half - 1])


def scale_block(blocks, gain_ref, scaled, count, width, owners):
    squares = None
    for j in range(count):
        rows = blocks[j].astype(F32)
        cols = slice(j * width, (j + 1) * width)
        scaled[:, cols] = (rows * gain_ref[:, cols]).astype(BF16)
        term = rows * rows
        squares = term if squares is None else squares + term
    total = jnp.sum(squares, axis=1, keepdims=True)
    rows = total.shape[0] // owners
    lane = lax.broadcasted_iota(jnp.int32, (rows, LANES), 1)
    spot = lax.broadcasted_iota(jnp.int32, (rows, LANES), 0)
    return [
        jnp.sum(
            jnp.where(lane == spot, total[o * rows : (o + 1) * rows], 0.0), axis=0, keepdims=True
        )
        for o in range(owners)
    ]


def split(value):
    high = value.astype(BF16).astype(F32)
    return high, value - high


def layer_kernel(
    n_kv, n_tp, features, parts_of,
    x_hbm, gain_a_hbm, gain_b_hbm, bound_hbm, head_gain_hbm,
    wq, wf, wi, wo, state_hbm, w_mix, w_gate, w_up, w_down,
    out_ref, state,
    xs, gain_a, gain_b, bound, head_gain, proj_w, state16, picks, fkv, mix_w, gate_w, down_w,
    blocks, scaled, squares, squares_in, raws, raws_in, normed, heads_all,
    sums, pair_in, joined, sums_in, mixed,
    parts, parts_in, hidden, hiddens,
    x_sem, small_sem, proj_sem, state_sem, w_sem,
    g_send, g_recv, q_send, q_recv, r_send, r_recv, n_send, n_recv,
    t_send, t_recv, p_send, p_recv, h_send, h_recv,
):
    halves = range(parts_of)
    _, seqs, width = xs.shape
    rows = seqs // n_kv
    n_heads, depth, wide = proj_w.shape
    dk = wide // 4
    units = gate_w.shape[1]
    half = n_tp // 2

    x_loads = []
    for h in halves:
        for o in range(n_kv):
            x_loads.append(pltpu.make_async_copy(
                x_hbm.at[pl.ds((o * parts_of + h) * rows, rows), :],
                xs.at[h, pl.ds(o * rows, rows), :], x_sem.at[h],
            ))
    small_loads = [
        pltpu.make_async_copy(source, target, small_sem.at[i])
        for i, (source, target) in enumerate((
            (gain_a_hbm, gain_a), (gain_b_hbm, gain_b), (bound_hbm, bound), (head_gain_hbm, head_gain),
        ))
    ]
    proj_loads = [
        [
            pltpu.make_async_copy(
                source.at[:, pl.ds(j * dk, dk)], proj_w.at[j, :, pl.ds(p * dk, dk)], proj_sem.at[j]
            )
            for p, source in enumerate((wq, wf, wi, wo))
        ]
        for j in range(n_heads)
    ]
    state_loads = [
        pltpu.make_async_copy(
            state_hbm.at[pl.ds(h * rows, rows)], state.at[pl.ds(h * rows, rows)], state_sem.at[h]
        )
        for h in halves
    ]
    w_loads = [
        pltpu.make_async_copy(source, target, w_sem.at[i])
        for i, (source, target) in enumerate(
            ((w_mix, mix_w), (w_gate, gate_w.at[0]), (w_up, gate_w.at[1]), (w_down, down_w))
        )
    ]
    for load in x_loads + small_loads + sum(proj_loads, []):
        load.start()

    kv, kv_peers = ring("kv", n_kv)
    me, core, chip, partner, _ = pairs(n_tp)
    own = pl.ds(pl.multiple_of(kv * rows, rows), rows)
    peer_rows = [pl.ds(pl.multiple_of(peer * rows, rows), rows) for peer in kv_peers]
    tp_peers = ring("tp", n_tp)[1]
    greet((("kv", kv_peers), ("tp", [partner] + tp_peers[1::2])))

    def send_squares(h, stage):
        sums_of = scale_block(
            blocks.at[stage, h], (gain_a, gain_b)[stage], scaled.at[stage, h], n_tp, width, n_kv
        )
        for o in range(n_kv):
            squares[stage, h, o] = sums_of[o]
        for i, peer in enumerate(kv_peers):
            remote(
                squares.at[stage, h, peer], squares_in.at[stage, h, i],
                q_send, q_recv.at[stage, h], "kv", peer,
            ).start()

    def inverse_of(h, stage):
        landed(squares_in.at[stage, h], q_recv.at[stage, h])
        total = squares[stage, h, pl.ds(kv, 1)][0]
        for i in range(n_kv - 1):
            total = total + squares_in[stage, h, i]
        lane = lax.broadcasted_iota(jnp.int32, (rows, LANES), 1)
        spot = lax.broadcasted_iota(jnp.int32, (rows, LANES), 0)
        total = jnp.sum(jnp.where(lane == spot, total, 0.0), axis=1, keepdims=True)
        return lax.rsqrt(total / features + EPS)

    def spread(h, source, target, send, recv):
        for peer in kv_peers:
            remote(source, target.at[h, own, :], send, recv.at[h], "kv", peer).start()
        target[h, own, :] = source[...]

    def others(target):
        return target.at[pl.ds(0, (n_kv - 1) * rows), :]

    group = max(1, 256 // width)
    while n_tp % group:
        group -= 1

    def start_reduce(h, stage, left, weight):
        for t in range(0, n_tp, group):
            part = jnp.dot(
                left[...], weight[:, t * width : (t + group) * width], preferred_element_type=F32
            ).astype(BF16)
            for j in range(group):
                sums[stage, h, (t + j) % 2, (t + j) // 2] = part[:, j * width : (j + 1) * width]
        first = remote(
            sums.at[stage, h, 1 - core], pair_in.at[stage, h],
            t_send.at[0], t_recv.at[stage, h, 0], "tp", partner,
        )
        first.start()
        return first

    def pair_sum(h, stage, place):
        mine = sums[stage, h, pl.ds(core, 1), pl.ds(place, 1)][0, 0].astype(F32)
        return mine + pair_in[stage, h, pl.ds(place, 1)][0].astype(F32)

    def join_reduce(h, stage, first):
        first.wait_recv()
        for i in range(1, half):
            joined[stage, h, i - 1] = pair_sum(h, stage, lax.rem(chip + i, half)).astype(BF16)
            remote(
                joined.at[stage, h, i - 1], sums_in.at[stage, h, i - 1],
                t_send.at[1], t_recv.at[stage, h, 1], "tp", lax.rem(me + 2 * i, n_tp),
            ).start()

    def end_reduce(h, stage, base):
        total = base + pair_sum(h, stage, chip)
        landed(sums_in.at[stage, h], t_recv.at[stage, h, 1])
        for i in range(half - 1):
            total = total + sums_in[stage, h, i].astype(F32)
        return total.astype(BF16)

    direct, firsts = {}, {}

    for h in halves:
        landed(xs.at[h], x_sem.at[h])
        direct[h] = start_gather(n_tp, xs.at[h], blocks.at[0, h], g_send.at[0], g_recv.at[0, h])
    place = lax.broadcasted_iota(jnp.int32, (4 * rows, 2 * dk), 0)
    lane = lax.broadcasted_iota(jnp.int32, (4 * rows, 2 * dk), 1)
    side = jnp.where((place < 2 * rows) == (lane < dk), 1.0, 0.0)
    owner = lax.rem(place, rows)
    for s in range(rows):
        picks[s] = jnp.where(owner == s, side, 0.0).astype(BF16)

    def update(h):
        def step(j, carry):
            left = jnp.concatenate(
                [*split(fkv[0, h, j]), *split(fkv[1, h, j])], axis=0
            ).T.astype(BF16)
            value = fkv[2, h, j]
            for s in range(rows):
                wide = jnp.dot(left, picks[s], preferred_element_type=F32)
                state[h * rows + s, j] = (
                    wide[:, :dk] * state[h * rows + s, j] + wide[:, dk:] * value[s : s + 1, :]
                )
            return carry
        lax.fori_loop(0, n_heads, step, 0)

    for load in small_loads:
        load.wait()
    for h in halves:
        relay_gather(n_tp, blocks.at[0, h], direct[h], g_send.at[0], g_recv.at[0, h])
    for load in state_loads:
        load.start()
    for h in halves:
        end_gather(n_tp, blocks.at[0, h], g_recv.at[0, h])
        send_squares(h, 0)
        for j in range(n_heads):
            if h == 0:
                landed(proj_w.at[j], proj_sem.at[j])
            raws[h, j] = jnp.dot(scaled[0, h], proj_w[j], preferred_element_type=F32).astype(BF16)
            for i, peer in enumerate(kv_peers):
                remote(
                    raws.at[h, j, peer_rows[i], :], raws_in.at[h, j, i],
                    r_send, r_recv.at[h, j], "kv", peer,
                ).start()

    for load in w_loads:
        load.start()

    def narrow(h):
        def step(j, carry):
            for s in range(rows):
                state16[h, j, :, s * dk : (s + 1) * dk] = state[h * rows + s, j].astype(BF16)
            return carry
        lax.fori_loop(0, n_heads, step, 0)

    for h in halves:
        state_loads[h].wait()
        narrow(h)
    spots = lax.broadcasted_iota(jnp.int32, (rows, dk), 0)
    for h in halves:
        inverse = inverse_of(h, 0)
        for j in range(n_heads):
            cols = slice(j * dk, (j + 1) * dk)
            total = raws[h, j, own, :].astype(F32)
            landed(raws_in.at[h, j], r_recv.at[h, j])
            for i in range(n_kv - 1):
                total = total + raws_in[h, j, i].astype(F32)
            total = total * inverse
            query, raw, value, gate = (total[:, p * dk : (p + 1) * dk] for p in range(4))
            low = bound[:, cols]
            forget = low + (1.0 - low) * jax.nn.sigmoid(raw)
            keyvec = (1.0 - low) * jax.nn.sigmoid(-raw)
            query = query * jax.nn.sigmoid(query)
            fkv[0, h, j] = forget
            fkv[1, h, j] = keyvec
            fkv[2, h, j] = value
            left = (query * forget).astype(BF16)
            head = jnp.sum(query * keyvec, axis=1, keepdims=True) * value
            seen = jnp.dot(left, state16[h, j], preferred_element_type=F32)
            for s in range(rows):
                head = head + jnp.where(spots == s, seen[:, s * dk : (s + 1) * dk], 0.0)
            scale = lax.rsqrt(jnp.mean(head * head, axis=1, keepdims=True) + EPS)
            normed[h, :, cols] = (
                head * scale * head_gain[...] * (gate * jax.nn.sigmoid(gate))
            ).astype(BF16)
        spread(h, normed.at[h], heads_all, n_send, n_recv)

    w_loads[0].wait()
    for h in halves:
        landed(others(heads_all.at[h]), n_recv.at[h])
        join_reduce(h, 0, start_reduce(h, 0, heads_all.at[h], mix_w))
    for h in halves:
        mixed[h] = end_reduce(h, 0, xs[h].astype(F32))
        direct[h] = start_gather(n_tp, mixed.at[h], blocks.at[1, h], g_send.at[1], g_recv.at[1, h])
        if h == 0:
            update(0)

    def relay(h):
        relay_gather(n_tp, blocks.at[1, h], direct[h], g_send.at[1], g_recv.at[1, h])

    relay(0)
    step = min(512, units)
    edges = [0, *range(step // 2, units - step // 2, step), units]
    chunks = list(zip(edges[:-1], edges[1:]))
    for h in halves:
        end_gather(n_tp, blocks.at[1, h], g_recv.at[1, h])
        send_squares(h, 1)
        for k, (c, end) in enumerate(chunks):
            for g in range(2):
                if h == 0 and k == 0:
                    w_loads[1 + g].wait()
                parts[h, g, :, c:end] = lax.dot_general(
                    scaled[1, h], gate_w[g, c:end, :], (((1,), (1,)), ((), ())),
                    preferred_element_type=F32,
                ).astype(BF16)
                for i, peer in enumerate(kv_peers):
                    remote(
                        parts.at[h, g, peer_rows[i], c:end], parts_in.at[h, i, g, :, c:end],
                        p_send, p_recv.at[h], "kv", peer,
                    ).start()
            if k == 1 and h + 1 < parts_of:
                relay(h + 1)
    for h in range(1, parts_of):
        update(h)
    for h in halves:
        inverse = inverse_of(h, 1)
        landed(parts_in.at[h], p_recv.at[h])
        both = []
        for g in range(2):
            total = parts[h, g, own, :].astype(F32)
            for i in range(n_kv - 1):
                total = total + parts_in[h, i, g].astype(F32)
            both.append(total * inverse)
        hidden[h] = (both[0] * jax.nn.sigmoid(both[0]) * both[1]).astype(BF16)
        spread(h, hidden.at[h], hiddens, h_send, h_recv)
    w_loads[3].wait()
    for h in halves:
        landed(others(hiddens.at[h]), h_recv.at[h])
        firsts[h] = start_reduce(h, 1, hiddens.at[h], down_w)
    for h in halves:
        join_reduce(h, 1, firsts[h])
    for h in halves:
        out_ref[h] = end_reduce(h, 1, mixed[h].astype(F32))
    for stage in range(2):
        landed(blocks.at[stage, :, pl.ds(0, n_tp - 1)], g_send.at[stage])
    for ref, sem in (
        (squares_in, q_send), (raws_in, r_send), (parts_in, p_send), (pair_in, t_send.at[0]), (sums_in, t_send.at[1]),
        (heads_all.at[:, pl.ds(0, (n_kv - 1) * rows)], n_send),
        (hiddens.at[:, pl.ds(0, (n_kv - 1) * rows)], h_send),
    ):
        landed(ref, sem)


def deliver_kernel(parts_of, n_kv, state_ref, part_ref, new_ref, out_ref, sems):
    local = state_ref.shape[0]
    rows = local // parts_of
    count = sems.shape[0]
    some = local // count
    copies = [
        pltpu.make_async_copy(
            state_ref.at[pl.ds(i * some, some)], new_ref.at[pl.ds(i * some, some)], sems.at[i]
        )
        for i in range(count)
    ]
    for copy in copies:
        copy.start()
    for h in range(parts_of):
        for o in range(n_kv):
            out_ref[pl.ds((o * parts_of + h) * rows, rows), :] = part_ref[h, pl.ds(o * rows, rows), :]
    for copy in copies:
        copy.wait()


def in_vmem():
    return pl.BlockSpec(memory_space=pltpu.VMEM)


def in_hbm():
    return pl.BlockSpec(memory_space=pltpu.HBM)


def body(
    n_kv, n_tp,
    residual, mixer_gain, w_query, w_forget, w_input, w_outgate, lower_bound, state,
    head_gain, w_mix_out, ffn_gain, w_gate, w_up, w_down,
):
    seqs, width = residual.shape
    depth, hid = w_query.shape
    local, n_heads, dk, dv = state.shape
    units = w_gate.shape[1]
    features = depth * n_kv
    half = n_tp // 2
    parts_of = 2 if local % 32 == 0 else 1
    rows = local // parts_of
    some = seqs // parts_of
    dma = pltpu.SemaphoreType.DMA
    stay = lambda array: pltpu.with_memory_space_constraint(array, pltpu.HBM)

    part, held = pl.pallas_call(
        functools.partial(layer_kernel, n_kv, n_tp, features, parts_of),
        out_shape=(
            jax.ShapeDtypeStruct((parts_of, some, width), BF16),
            jax.ShapeDtypeStruct(state.shape, F32),
        ),
        in_specs=[in_hbm()] * 14,
        out_specs=(in_vmem(), in_vmem()),
        scratch_shapes=[
            pltpu.VMEM((parts_of, some, width), BF16),
            pltpu.VMEM((1, depth), F32),
            pltpu.VMEM((1, depth), F32),
            pltpu.VMEM((1, hid), F32),
            pltpu.VMEM((1, dv), F32),
            pltpu.VMEM((n_heads, depth, 4 * dk), BF16),
            pltpu.VMEM((parts_of, n_heads, dk, rows * dv), BF16),
            pltpu.VMEM((rows, 4 * rows, 2 * dk), BF16),
            pltpu.VMEM((3, parts_of, n_heads, rows, dk), F32),
            pltpu.VMEM(w_mix_out.shape, BF16),
            pltpu.VMEM((2, units, depth), BF16),
            pltpu.VMEM(w_down.shape, BF16),
            pltpu.VMEM((2, parts_of, n_tp, some, width), BF16),
            pltpu.VMEM((2, parts_of, some, depth), BF16),
            pltpu.VMEM((2, parts_of, n_kv, 1, LANES), F32),
            pltpu.VMEM((2, parts_of, n_kv - 1, 1, LANES), F32),
            pltpu.VMEM((parts_of, n_heads, some, 4 * dk), BF16),
            pltpu.VMEM((parts_of, n_heads, n_kv - 1, rows, 4 * dk), BF16),
            pltpu.VMEM((parts_of, rows, hid), BF16),
            pltpu.VMEM((parts_of, some, hid), BF16),
            pltpu.VMEM((2, parts_of, 2, half, some, width), BF16),
            pltpu.VMEM((2, parts_of, half, some, width), BF16),
            pltpu.VMEM((2, parts_of, half - 1, some, width), BF16),
            pltpu.VMEM((2, parts_of, half - 1, some, width), BF16),
            pltpu.VMEM((parts_of, some, width), BF16),
            pltpu.VMEM((parts_of, 2, some, units), BF16),
            pltpu.VMEM((parts_of, n_kv - 1, 2, rows, units), BF16),
            pltpu.VMEM((parts_of, rows, units), BF16),
            pltpu.VMEM((parts_of, some, units), BF16),
            dma((parts_of,)), dma((4,)), dma((n_heads,)), dma((parts_of,)), dma((4,)),
            dma((2,)), dma((2, parts_of, half)),
            dma, dma((2, parts_of)),
            dma, dma((parts_of, n_heads)),
            dma, dma((parts_of,)),
            dma((2,)), dma((2, parts_of, 2)),
            dma, dma((parts_of,)),
            dma, dma((parts_of,)),
        ],
        compiler_params=pltpu.CompilerParams(
            collective_id=0, has_side_effects=True, vmem_limit_bytes=44 * 2**20
        ),
        name="layer",
    )(*map(stay, (
        residual, mixer_gain.reshape(1, depth), ffn_gain.reshape(1, depth),
        lower_bound.reshape(1, hid), head_gain.reshape(1, dv),
        w_query, w_forget, w_input, w_outgate, state, w_mix_out, w_gate.T, w_up.T, w_down,
    )))

    held = pltpu.with_memory_space_constraint(held, pltpu.VMEM)
    updated, layer_out = pl.pallas_call(
        functools.partial(deliver_kernel, parts_of, n_kv),
        out_shape=(
            jax.ShapeDtypeStruct(state.shape, F32),
            jax.ShapeDtypeStruct((seqs, width), BF16),
        ),
        in_specs=[in_vmem()] * 2,
        out_specs=(in_hbm(), in_vmem()),
        scratch_shapes=[dma((8 if local % 8 == 0 else 1,))],
        compiler_params=pltpu.CompilerParams(vmem_limit_bytes=16 * 2**20),
        name="deliver",
    )(held, part)
    return layer_out, updated


def solution(mesh):
    in_specs = (
        P(None, ("kv", "tp")),
        P("kv"),
        P("kv", "tp"),
        P("kv", "tp"),
        P("kv", "tp"),
        P("kv", "tp"),
        P("tp"),
        P("kv", "tp", None, None),
        P(),
        P("tp", "kv"),
        P("kv"),
        P("kv", "tp"),
        P("kv", "tp"),
        P("tp", "kv"),
    )
    out_specs = (P(None, ("kv", "tp")), P("kv", "tp", None, None))
    return jax.shard_map(
        functools.partial(body, mesh.shape["kv"], mesh.shape["tp"]),
        mesh=mesh, in_specs=in_specs, out_specs=out_specs, check_vma=False,
    )
```

```python
import functools

import jax
import jax.numpy as jnp
from jax import lax
from jax.experimental import pallas as pl
from jax.experimental.pallas import tpu as pltpu
from jax.sharding import PartitionSpec as P

EPS = 1e-06
F32 = jnp.float32
BF16 = jnp.bfloat16
LANES = 128


def ring(axis, size):
    me = lax.axis_index(axis)
    return me, [lax.rem(me + step, size) for step in range(1, size)]


def greet(axes):
    barrier = pltpu.get_barrier_semaphore()
    count = 0
    for axis, peers in axes:
        for peer in peers:
            pl.semaphore_signal(
                barrier, inc=1, device_id={axis: peer}, device_id_type=pl.DeviceIdType.MESH
            )
            count += 1
    pl.semaphore_wait(barrier, count)


def remote(source, target, send_sem, recv_sem, axis, peer):
    return pltpu.make_async_remote_copy(
        src_ref=source,
        dst_ref=target,
        send_sem=send_sem,
        recv_sem=recv_sem,
        device_id={axis: peer},
        device_id_type=pl.DeviceIdType.MESH,
    )


def pairs(n_tp):
    me = lax.axis_index("tp")
    core = lax.rem(me, 2)
    return me, core, lax.div(me, 2), me + 1 - 2 * core, n_tp // 2


def landed(ref, sem):
    pltpu.make_async_copy(ref, ref, sem).wait()


def start_gather(n_tp, source, blocks, send, recv):
    me, _, _, partner, half = pairs(n_tp)
    targets = [lax.rem(me + 2 * i, n_tp) for i in range(1, half)] + [partner]
    direct = [
        remote(source, blocks.at[me], send, recv.at[i], "tp", target)
        for i, target in enumerate(targets)
    ]
    for copy in direct:
        copy.start()
    blocks[pl.ds(me, 1)] = source[...][None]
    return direct


def relay_gather(n_tp, blocks, direct, send, recv):
    me, _, _, partner, half = pairs(n_tp)
    for i in range(1, half):
        origin = lax.rem(me - 2 * i + n_tp, n_tp)
        direct[i - 1].wait_recv()
        remote(
            blocks.at[origin], blocks.at[origin], send, recv.at[half - 1], "tp", partner
        ).start()


def end_gather(n_tp, blocks, recv):
    half = n_tp // 2
    landed(blocks.at[pl.ds(0, half)], recv.at[half - 1])


def scale_block(blocks, gain_ref, scaled, count, width, owners):
    squares = None
    for j in range(count):
        rows = blocks[j].astype(F32)
        cols = slice(j * width, (j + 1) * width)
        scaled[:, cols] = (rows * gain_ref[:, cols]).astype(BF16)
        term = rows * rows
        squares = term if squares is None else squares + term
    total = jnp.sum(squares, axis=1, keepdims=True)
    rows = total.shape[0] // owners
    lane = lax.broadcasted_iota(jnp.int32, (rows, LANES), 1)
    spot = lax.broadcasted_iota(jnp.int32, (rows, LANES), 0)
    return [
        jnp.sum(
            jnp.where(lane == spot, total[o * rows : (o + 1) * rows], 0.0), axis=0, keepdims=True
        )
        for o in range(owners)
    ]


def split(value):
    high = value.astype(BF16).astype(F32)
    return high, value - high


def layer_kernel(
    n_kv, n_tp, features, parts_of,
    x_hbm, gain_a_hbm, gain_b_hbm, bound_hbm, head_gain_hbm,
    wq, wf, wi, wo, state_hbm, w_mix, w_gate, w_up, w_down,
    out_ref, state,
    xs, gain_a, gain_b, bound, head_gain, proj_w, state16, picks, fkv, mix_w, gate_w, down_w,
    blocks, scaled, squares, squares_in, raws, raws_in, normed, heads_all,
    sums, pair_in, joined, sums_in, mixed,
    parts, parts_in, hidden, hiddens,
    x_sem, small_sem, proj_sem, state_sem, w_sem,
    g_send, g_recv, q_send, q_recv, r_send, r_recv, n_send, n_recv,
    t_send, t_recv, p_send, p_recv, h_send, h_recv,
):
    halves = range(parts_of)
    _, seqs, width = xs.shape
    rows = seqs // n_kv
    n_heads, depth, wide = proj_w.shape
    dk = wide // 4
    units = gate_w.shape[1]
    half = n_tp // 2

    x_loads = []
    for h in halves:
        for o in range(n_kv):
            x_loads.append(pltpu.make_async_copy(
                x_hbm.at[pl.ds((o * parts_of + h) * rows, rows), :],
                xs.at[h, pl.ds(o * rows, rows), :], x_sem.at[h],
            ))
    small_loads = [
        pltpu.make_async_copy(source, target, small_sem.at[i])
        for i, (source, target) in enumerate((
            (gain_a_hbm, gain_a), (gain_b_hbm, gain_b), (bound_hbm, bound), (head_gain_hbm, head_gain),
        ))
    ]
    proj_loads = [
        [
            pltpu.make_async_copy(
                source.at[:, pl.ds(j * dk, dk)], proj_w.at[j, :, pl.ds(p * dk, dk)], proj_sem.at[j]
            )
            for p, source in enumerate((wq, wf, wi, wo))
        ]
        for j in range(n_heads)
    ]
    state_loads = [
        pltpu.make_async_copy(
            state_hbm.at[pl.ds(h * rows, rows)], state.at[pl.ds(h * rows, rows)], state_sem.at[h]
        )
        for h in halves
    ]
    w_loads = [
        pltpu.make_async_copy(source, target, w_sem.at[i])
        for i, (source, target) in enumerate(
            ((w_mix, mix_w), (w_gate, gate_w.at[0]), (w_up, gate_w.at[1]), (w_down, down_w))
        )
    ]
    for load in x_loads + small_loads:
        load.start()

    kv, kv_peers = ring("kv", n_kv)
    me, core, chip, partner, _ = pairs(n_tp)
    own = pl.ds(pl.multiple_of(kv * rows, rows), rows)
    peer_rows = [pl.ds(pl.multiple_of(peer * rows, rows), rows) for peer in kv_peers]
    tp_peers = ring("tp", n_tp)[1]
    greet((("kv", kv_peers), ("tp", [partner] + tp_peers[1::2])))

    def send_squares(h, stage):
        sums_of = scale_block(
            blocks.at[stage, h], (gain_a, gain_b)[stage], scaled.at[stage, h], n_tp, width, n_kv
        )
        for o in range(n_kv):
            squares[stage, h, o] = sums_of[o]
        for i, peer in enumerate(kv_peers):
            remote(
                squares.at[stage, h, peer], squares_in.at[stage, h, i],
                q_send, q_recv.at[stage, h], "kv", peer,
            ).start()

    def inverse_of(h, stage):
        landed(squares_in.at[stage, h], q_recv.at[stage, h])
        total = squares[stage, h, pl.ds(kv, 1)][0]
        for i in range(n_kv - 1):
            total = total + squares_in[stage, h, i]
        lane = lax.broadcasted_iota(jnp.int32, (rows, LANES), 1)
        spot = lax.broadcasted_iota(jnp.int32, (rows, LANES), 0)
        total = jnp.sum(jnp.where(lane == spot, total, 0.0), axis=1, keepdims=True)
        return lax.rsqrt(total / features + EPS)

    def spread(h, source, target, send, recv):
        for peer in kv_peers:
            remote(source, target.at[h, own, :], send, recv.at[h], "kv", peer).start()
        target[h, own, :] = source[...]

    def others(target):
        return target.at[pl.ds(0, (n_kv - 1) * rows), :]

    group = max(1, 256 // width)
    while n_tp % group:
        group -= 1

    def start_reduce(h, stage, left, weight):
        for t in range(0, n_tp, group):
            part = jnp.dot(
                left[...], weight[:, t * width : (t + group) * width], preferred_element_type=F32
            ).astype(BF16)
            for j in range(group):
                sums[stage, h, (t + j) % 2, (t + j) // 2] = part[:, j * width : (j + 1) * width]
        first = remote(
            sums.at[stage, h, 1 - core], pair_in.at[stage, h],
            t_send.at[0], t_recv.at[stage, h, 0], "tp", partner,
        )
        first.start()
        return first

    def pair_sum(h, stage, place):
        mine = sums[stage, h, pl.ds(core, 1), pl.ds(place, 1)][0, 0].astype(F32)
        return mine + pair_in[stage, h, pl.ds(place, 1)][0].astype(F32)

    def join_reduce(h, stage, first):
        first.wait_recv()
        for i in range(1, half):
            joined[stage, h, i - 1] = pair_sum(h, stage, lax.rem(chip + i, half)).astype(BF16)
            remote(
                joined.at[stage, h, i - 1], sums_in.at[stage, h, i - 1],
                t_send.at[1], t_recv.at[stage, h, 1], "tp", lax.rem(me + 2 * i, n_tp),
            ).start()

    def end_reduce(h, stage, base):
        total = base + pair_sum(h, stage, chip)
        landed(sums_in.at[stage, h], t_recv.at[stage, h, 1])
        for i in range(half - 1):
            total = total + sums_in[stage, h, i].astype(F32)
        return total.astype(BF16)

    direct, firsts = {}, {}

    for h in halves:
        landed(xs.at[h], x_sem.at[h])
        direct[h] = start_gather(n_tp, xs.at[h], blocks.at[0, h], g_send.at[0], g_recv.at[0, h])
    for load in sum(proj_loads, []):
        load.start()
    place = lax.broadcasted_iota(jnp.int32, (4 * rows, 2 * dk), 0)
    lane = lax.broadcasted_iota(jnp.int32, (4 * rows, 2 * dk), 1)
    side = jnp.where((place < 2 * rows) == (lane < dk), 1.0, 0.0)
    owner = lax.rem(place, rows)
    for s in range(rows):
        picks[s] = jnp.where(owner == s, side, 0.0).astype(BF16)

    def update(h):
        def step(j, carry):
            left = jnp.concatenate(
                [*split(fkv[0, h, j]), *split(fkv[1, h, j])], axis=0
            ).T.astype(BF16)
            value = fkv[2, h, j]
            for s in range(rows):
                wide = jnp.dot(left, picks[s], preferred_element_type=F32)
                state[h * rows + s, j] = (
                    wide[:, :dk] * state[h * rows + s, j] + wide[:, dk:] * value[s : s + 1, :]
                )
            return carry
        lax.fori_loop(0, n_heads, step, 0)

    for load in small_loads:
        load.wait()
    for h in halves:
        relay_gather(n_tp, blocks.at[0, h], direct[h], g_send.at[0], g_recv.at[0, h])
    for load in state_loads:
        load.start()
    for h in halves:
        end_gather(n_tp, blocks.at[0, h], g_recv.at[0, h])
        send_squares(h, 0)
        for j in range(n_heads):
            if h == 0:
                landed(proj_w.at[j], proj_sem.at[j])
            raws[h, j] = jnp.dot(scaled[0, h], proj_w[j], preferred_element_type=F32).astype(BF16)
            for i, peer in enumerate(kv_peers):
                remote(
                    raws.at[h, j, peer_rows[i], :], raws_in.at[h, j, i],
                    r_send, r_recv.at[h, j], "kv", peer,
                ).start()

    for load in w_loads:
        load.start()

    def narrow(h):
        def step(j, carry):
            for s in range(rows):
                state16[h, j, :, s * dk : (s + 1) * dk] = state[h * rows + s, j].astype(BF16)
            return carry
        lax.fori_loop(0, n_heads, step, 0)

    for h in halves:
        state_loads[h].wait()
        narrow(h)
    spots = lax.broadcasted_iota(jnp.int32, (rows, dk), 0)
    for h in halves:
        inverse = inverse_of(h, 0)
        for j in range(n_heads):
            cols = slice(j * dk, (j + 1) * dk)
            total = raws[h, j, own, :].astype(F32)
            landed(raws_in.at[h, j], r_recv.at[h, j])
            for i in range(n_kv - 1):
                total = total + raws_in[h, j, i].astype(F32)
            total = total * inverse
            query, raw, value, gate = (total[:, p * dk : (p + 1) * dk] for p in range(4))
            low = bound[:, cols]
            forget = low + (1.0 - low) * jax.nn.sigmoid(raw)
            keyvec = (1.0 - low) * jax.nn.sigmoid(-raw)
            query = query * jax.nn.sigmoid(query)
            fkv[0, h, j] = forget
            fkv[1, h, j] = keyvec
            fkv[2, h, j] = value
            left = (query * forget).astype(BF16)
            head = jnp.sum(query * keyvec, axis=1, keepdims=True) * value
            seen = jnp.dot(left, state16[h, j], preferred_element_type=F32)
            for s in range(rows):
                head = head + jnp.where(spots == s, seen[:, s * dk : (s + 1) * dk], 0.0)
            scale = lax.rsqrt(jnp.mean(head * head, axis=1, keepdims=True) + EPS)
            normed[h, :, cols] = (
                head * scale * head_gain[...] * (gate * jax.nn.sigmoid(gate))
            ).astype(BF16)
        spread(h, normed.at[h], heads_all, n_send, n_recv)

    w_loads[0].wait()
    for h in halves:
        landed(others(heads_all.at[h]), n_recv.at[h])
        join_reduce(h, 0, start_reduce(h, 0, heads_all.at[h], mix_w))
    for h in halves:
        mixed[h] = end_reduce(h, 0, xs[h].astype(F32))
        direct[h] = start_gather(n_tp, mixed.at[h], blocks.at[1, h], g_send.at[1], g_recv.at[1, h])
        if h == 0:
            update(0)

    def relay(h):
        relay_gather(n_tp, blocks.at[1, h], direct[h], g_send.at[1], g_recv.at[1, h])

    relay(0)
    step = min(512, units)
    edges = [0, *range(step // 2, units - step // 2, step), units]
    chunks = list(zip(edges[:-1], edges[1:]))
    for h in halves:
        end_gather(n_tp, blocks.at[1, h], g_recv.at[1, h])
        send_squares(h, 1)
        for k, (c, end) in enumerate(chunks):
            for g in range(2):
                if h == 0 and k == 0:
                    w_loads[1 + g].wait()
                parts[h, g, :, c:end] = lax.dot_general(
                    scaled[1, h], gate_w[g, c:end, :], (((1,), (1,)), ((), ())),
                    preferred_element_type=F32,
                ).astype(BF16)
                for i, peer in enumerate(kv_peers):
                    remote(
                        parts.at[h, g, peer_rows[i], c:end], parts_in.at[h, i, g, :, c:end],
                        p_send, p_recv.at[h], "kv", peer,
                    ).start()
            if k == 1 and h + 1 < parts_of:
                relay(h + 1)
    for h in range(1, parts_of):
        update(h)
    for h in halves:
        inverse = inverse_of(h, 1)
        landed(parts_in.at[h], p_recv.at[h])
        both = []
        for g in range(2):
            total = parts[h, g, own, :].astype(F32)
            for i in range(n_kv - 1):
                total = total + parts_in[h, i, g].astype(F32)
            both.append(total * inverse)
        hidden[h] = (both[0] * jax.nn.sigmoid(both[0]) * both[1]).astype(BF16)
        spread(h, hidden.at[h], hiddens, h_send, h_recv)
    w_loads[3].wait()
    for h in halves:
        landed(others(hiddens.at[h]), h_recv.at[h])
        firsts[h] = start_reduce(h, 1, hiddens.at[h], down_w)
    for h in halves:
        join_reduce(h, 1, firsts[h])
    for h in halves:
        out_ref[h] = end_reduce(h, 1, mixed[h].astype(F32))
    for stage in range(2):
        landed(blocks.at[stage, :, pl.ds(0, n_tp - 1)], g_send.at[stage])
    for ref, sem in (
        (squares_in, q_send), (raws_in, r_send), (parts_in, p_send), (pair_in, t_send.at[0]), (sums_in, t_send.at[1]),
        (heads_all.at[:, pl.ds(0, (n_kv - 1) * rows)], n_send),
        (hiddens.at[:, pl.ds(0, (n_kv - 1) * rows)], h_send),
    ):
        landed(ref, sem)


def deliver_kernel(parts_of, n_kv, state_ref, part_ref, new_ref, out_ref, sems):
    local = state_ref.shape[0]
    rows = local // parts_of
    count = sems.shape[0]
    some = local // count
    copies = [
        pltpu.make_async_copy(
            state_ref.at[pl.ds(i * some, some)], new_ref.at[pl.ds(i * some, some)], sems.at[i]
        )
        for i in range(count)
    ]
    for copy in copies:
        copy.start()
    for h in range(parts_of):
        for o in range(n_kv):
            out_ref[pl.ds((o * parts_of + h) * rows, rows), :] = part_ref[h, pl.ds(o * rows, rows), :]
    for copy in copies:
        copy.wait()


def in_vmem():
    return pl.BlockSpec(memory_space=pltpu.VMEM)


def in_hbm():
    return pl.BlockSpec(memory_space=pltpu.HBM)


def body(
    n_kv, n_tp,
    residual, mixer_gain, w_query, w_forget, w_input, w_outgate, lower_bound, state,
    head_gain, w_mix_out, ffn_gain, w_gate, w_up, w_down,
):
    seqs, width = residual.shape
    depth, hid = w_query.shape
    local, n_heads, dk, dv = state.shape
    units = w_gate.shape[1]
    features = depth * n_kv
    half = n_tp // 2
    parts_of = 2 if local % 32 == 0 else 1
    rows = local // parts_of
    some = seqs // parts_of
    dma = pltpu.SemaphoreType.DMA
    stay = lambda array: pltpu.with_memory_space_constraint(array, pltpu.HBM)

    part, held = pl.pallas_call(
        functools.partial(layer_kernel, n_kv, n_tp, features, parts_of),
        out_shape=(
            jax.ShapeDtypeStruct((parts_of, some, width), BF16),
            jax.ShapeDtypeStruct(state.shape, F32),
        ),
        in_specs=[in_hbm()] * 14,
        out_specs=(in_vmem(), in_vmem()),
        scratch_shapes=[
            pltpu.VMEM((parts_of, some, width), BF16),
            pltpu.VMEM((1, depth), F32),
            pltpu.VMEM((1, depth), F32),
            pltpu.VMEM((1, hid), F32),
            pltpu.VMEM((1, dv), F32),
            pltpu.VMEM((n_heads, depth, 4 * dk), BF16),
            pltpu.VMEM((parts_of, n_heads, dk, rows * dv), BF16),
            pltpu.VMEM((rows, 4 * rows, 2 * dk), BF16),
            pltpu.VMEM((3, parts_of, n_heads, rows, dk), F32),
            pltpu.VMEM(w_mix_out.shape, BF16),
            pltpu.VMEM((2, units, depth), BF16),
            pltpu.VMEM(w_down.shape, BF16),
            pltpu.VMEM((2, parts_of, n_tp, some, width), BF16),
            pltpu.VMEM((2, parts_of, some, depth), BF16),
            pltpu.VMEM((2, parts_of, n_kv, 1, LANES), F32),
            pltpu.VMEM((2, parts_of, n_kv - 1, 1, LANES), F32),
            pltpu.VMEM((parts_of, n_heads, some, 4 * dk), BF16),
            pltpu.VMEM((parts_of, n_heads, n_kv - 1, rows, 4 * dk), BF16),
            pltpu.VMEM((parts_of, rows, hid), BF16),
            pltpu.VMEM((parts_of, some, hid), BF16),
            pltpu.VMEM((2, parts_of, 2, half, some, width), BF16),
            pltpu.VMEM((2, parts_of, half, some, width), BF16),
            pltpu.VMEM((2, parts_of, half - 1, some, width), BF16),
            pltpu.VMEM((2, parts_of, half - 1, some, width), BF16),
            pltpu.VMEM((parts_of, some, width), BF16),
            pltpu.VMEM((parts_of, 2, some, units), BF16),
            pltpu.VMEM((parts_of, n_kv - 1, 2, rows, units), BF16),
            pltpu.VMEM((parts_of, rows, units), BF16),
            pltpu.VMEM((parts_of, some, units), BF16),
            dma((parts_of,)), dma((4,)), dma((n_heads,)), dma((parts_of,)), dma((4,)),
            dma((2,)), dma((2, parts_of, half)),
            dma, dma((2, parts_of)),
            dma, dma((parts_of, n_heads)),
            dma, dma((parts_of,)),
            dma((2,)), dma((2, parts_of, 2)),
            dma, dma((parts_of,)),
            dma, dma((parts_of,)),
        ],
        compiler_params=pltpu.CompilerParams(
            collective_id=0, has_side_effects=True, vmem_limit_bytes=44 * 2**20
        ),
        name="layer",
    )(*map(stay, (
        residual, mixer_gain.reshape(1, depth), ffn_gain.reshape(1, depth),
        lower_bound.reshape(1, hid), head_gain.reshape(1, dv),
        w_query, w_forget, w_input, w_outgate, state, w_mix_out, w_gate.T, w_up.T, w_down,
    )))

    held = pltpu.with_memory_space_constraint(held, pltpu.VMEM)
    updated, layer_out = pl.pallas_call(
        functools.partial(deliver_kernel, parts_of, n_kv),
        out_shape=(
            jax.ShapeDtypeStruct(state.shape, F32),
            jax.ShapeDtypeStruct((seqs, width), BF16),
        ),
        in_specs=[in_vmem()] * 2,
        out_specs=(in_hbm(), in_vmem()),
        scratch_shapes=[dma((8 if local % 8 == 0 else 1,))],
        compiler_params=pltpu.CompilerParams(vmem_limit_bytes=16 * 2**20),
        name="deliver",
    )(held, part)
    return layer_out, updated


def solution(mesh):
    in_specs = (
        P(None, ("kv", "tp")),
        P("kv"),
        P("kv", "tp"),
        P("kv", "tp"),
        P("kv", "tp"),
        P("kv", "tp"),
        P("tp"),
        P("kv", "tp", None, None),
        P(),
        P("tp", "kv"),
        P("kv"),
        P("kv", "tp"),
        P("kv", "tp"),
        P("tp", "kv"),
    )
    out_specs = (P(None, ("kv", "tp")), P("kv", "tp", None, None))
    return jax.shard_map(
        functools.partial(body, mesh.shape["kv"], mesh.shape["tp"]),
        mesh=mesh, in_specs=in_specs, out_specs=out_specs, check_vma=False,
    )
```
